32 devices in a mesh: ep: 8 (over z, x), tp: 4 (over y, core).
Axes of the slice: x: 2, y: 2, z: 4, core: 2. Of those that a mesh axis runs over, the one named last changes fastest.
Arguments:
- tokens: bfloat16 [64, 4096], P(('ep', 'tp')), may hold values from -6 to 6
- lengths: int32 [64], P('ep'), may hold values from 64 to 1024, as said below
- latent_cache: bfloat16 [64, 1024, 256], P(('ep', 'tp')), may hold values from -6 to 6
- rope_cache: bfloat16 [64, 1024, 64], P(('ep', 'tp')), may hold values from -1200 to 1200
- attn_gain: bfloat16 [4096], replicated, may hold values from 0.099609375 to 1.8984375
- query_weight: bfloat16 [4096, 2048], P(None, 'tp'), may hold values from -0.09375 to 0.09375
- query_rot_weight: bfloat16 [4096, 1024], P(None, 'tp'), may hold values from -0.09375 to 0.09375
- latent_weight: bfloat16 [4096, 256], P('tp'), may hold values from -0.09375 to 0.09375
- key_rot_weight: bfloat16 [4096, 64], P('tp'), may hold values from -0.09375 to 0.09375
- latent_gain: bfloat16 [256], replicated, may hold values from 0.099609375 to 1.8984375
- absorb_weight: bfloat16 [16, 128, 256], P('tp'), may hold values from -0.5 to 0.5
- value_weight: bfloat16 [16, 256, 128], P('tp'), may hold values from -0.375 to 0.375
- output_weight: bfloat16 [2048, 4096], P('tp'), may hold values from -0.125 to 0.125
- mix_gain: bfloat16 [4096], replicated, may hold values from 0.099609375 to 1.8984375
- expert_gain: bfloat16 [4096], replicated, may hold values from 0.099609375 to 1.8984375
- gate_weight: bfloat16 [8, 4096, 512], P('ep', None, 'tp'), may hold values from -0.09375 to 0.09375
- up_weight: bfloat16 [8, 4096, 512], P('ep', None, 'tp'), may hold values from -0.09375 to 0.09375
- down_weight: bfloat16 [8, 512, 4096], P('ep', 'tp'), may hold values from -0.25 to 0.25
- expert_ids: int32 [64, 2], P('ep'), may hold values from 0 to 7, all different within a row; in each aligned block of 8 rows (0 to 7, 8 to 15, ...) at most 4 rows name the same one
- route_weights: float32 [64, 2], P('ep'), may hold values from 0.2 to 1
Outputs:
- out: bfloat16 [64, 4096], P('ep', 'tp')
- new_latent: bfloat16 [64, 256], P(('ep', 'tp'))
- new_rope: bfloat16 [64, 64], P(('ep', 'tp'))
The draws below stay inside these ranges and needn't reach their ends.
Inputs may be any that keep to these rules, and one draw needn't show every extreme that they name: The new token sits at position lengths[b]; some sequence has exactly 1024. `expert_ids`: the experts of a row differ; among the rows of one index of ep no expert is named by more than 4 rows, a bound that some block reaches there.
All inputs are finite; a program needn't handle non-finite values.
Results may differ from the reference program's by a relative error of at most 0.023.
Values may be sent and summed in bfloat16 or wider, within the bound.
A program may use at most 64 MiB of HBM per device.

```python
import math
import jax
import jax.numpy as jnp
import numpy as np
from jax import lax

D = 4096
HEADS = 16
QK_NOPE = 128
QK_ROPE = 64
VALUE_DIM = 128
LATENT = 256
FF = 512
TOPK = 2
SEQ_DEV = 2
CTX = 1024
BATCH = 64
EXPERTS = 8
CAP = 4
N_EP = 8
N_TP = 4


def draw_lengths(key, part):
    level_key, extra_key, full_key = jax.random.split(key, 3)
    level = jax.random.randint(level_key, (BATCH,), 1, 5)
    floor_len = jnp.right_shift(jnp.full((BATCH,), CTX, jnp.int32), level)
    extra = jax.random.randint(extra_key, (BATCH,), 0, CTX + 1) % (floor_len + 1)
    chosen = jax.random.randint(full_key, (), 0, BATCH)
    values = jnp.where(jnp.arange(BATCH) == chosen, CTX, floor_len + extra)
    return values.astype(jnp.int32)


def draw_rope_cache(key, part):
    normal_key, planted_key = jax.random.split(key)
    values = jnp.clip(jax.random.normal(normal_key, (BATCH, CTX, QK_ROPE), jnp.float32), -6.0, 6.0)
    return values.astype(jnp.bfloat16)


def level_of(key, dims, shards, least, largest):
    level = 1.0
    for dim, shards_of in shards:
        steps = jax.random.uniform(jax.random.fold_in(jax.random.fold_in(key, 6), dim), (shards_of,), jnp.float32, least / len(shards), largest / len(shards))
        level = level * jnp.repeat(jnp.exp(steps), dims[dim] // shards_of).reshape((-1,) + (1,) * (len(dims) - 1 - dim))
    return level


def routed_block(rng, own, number, rows, amount, top, limit, skew):
    order = jax.random.permutation(rng, amount)
    crowded, common = shares(amount, rows * top, limit, skew, True), shares(amount, rows * top, limit, skew, False)
    places = jnp.arange(amount)

    def named(sizes, rotation):
        used = int((sizes > 0).sum())
        fixed = max(1, used // 4)
        passed = fixed + (places - fixed + rotation * (used - fixed)) % max(1, amount - fixed)
        return jnp.zeros((amount,), jnp.int32).at[order[jnp.where(places < fixed, places, passed)]].set(jnp.asarray(sizes, jnp.int32))

    sizes = jnp.where(number % 4 == 0, named(crowded, number // 4), named(common, number - number // 4 - 1))
    mixed = jax.random.permutation(jax.random.fold_in(own, 3), amount)
    source_of, receiver = mixed[0:amount // 2 * 2:2], mixed[1:amount // 2 * 2:2]
    slack = jnp.minimum(sizes[source_of] - 1, limit - sizes[receiver]) // 2
    slack = jnp.where((source_of == order[0]) | (receiver == order[0]) | (sizes[receiver] == 0), 0, jnp.maximum(slack, 0))
    passed = jax.random.randint(jax.random.fold_in(own, 4), (amount // 2,), 0, 1 << 20) % (slack + 1)
    sizes = sizes.at[source_of].add(-passed).at[receiver].add(passed)
    members = jnp.searchsorted(jnp.cumsum(sizes), jnp.arange(rows * top), side="right").astype(jnp.int32)
    table = members.reshape(top, rows).T
    table = table[jax.random.permutation(jax.random.fold_in(own, 1), rows)]
    rotation = jax.random.randint(jax.random.fold_in(own, 2), (rows, 1), 0, top)
    return jnp.take_along_axis(table, (jnp.arange(top)[None, :] + rotation) % top, axis=1)


def shares(amount, total, bound, skew, full):
    weights = [(1 << 20) // math.isqrt(standing ** skew) + 1 for standing in range(1, amount + 1)]
    largest = bound if full else min(bound, max(-(-total // amount), total * weights[0] // sum(weights)))
    least = 1 if total - largest >= amount - 1 else 0
    counts, spare = [largest] + [least] * (amount - 1), total - largest - least * (amount - 1)
    while spare > 0:
        candidates = [i for i in range(1, amount) if counts[i] < largest] or [i for i in range(1, amount) if counts[i] < bound]
        pool, budget = sum([weights[i] for i in candidates]), spare
        for i in candidates:
            more = min(bound - counts[i], max(1, budget * weights[i] // pool), spare)
            counts[i] = counts[i] + more
            spare = spare - more
    return np.array(counts)


def bell_draw(stream_key, dims, scale, limit, cuts=(), kind=jnp.bfloat16):
    result = jax.random.normal(stream_key, dims, jnp.float32) * scale
    if len(cuts) > 0:
        result = level_of(stream_key, dims, cuts, -0.22, 0.18) * result
    return jnp.clip(result, min=-limit, max=limit).astype(kind)


def setup_inputs(seed: int = 0) -> dict:
    splits = jax.random.split(jax.random.key(seed), 21)
    tokens = bell_draw(splits[0], (BATCH, D), 1.0, 6.0, ((0, 32),))
    lengths = draw_lengths(jax.random.fold_in(splits[20], 71), 0)
    latent_cache = bell_draw(splits[2], (BATCH, CTX, LATENT), 1.0, 6.0, ((0, 32),))
    rope_cache = draw_rope_cache(jax.random.fold_in(splits[20], 71), 0)
    attn_gain = jnp.clip(1.0 + 0.18 * jax.random.normal(splits[4], (D,), jnp.float32), 0.099609375, 1.8984375).astype(jnp.bfloat16)
    query_weight = bell_draw(splits[5], (D, HEADS * QK_NOPE), D ** -0.5, 0.09375, ((1, 4),))
    query_rot_weight = bell_draw(splits[6], (D, HEADS * QK_ROPE), D ** -0.5, 0.09375, ((1, 4),))
    latent_weight = bell_draw(splits[7], (D, LATENT), D ** -0.5, 0.09375, ((0, 4),))
    key_rot_weight = bell_draw(splits[8], (D, QK_ROPE), D ** -0.5, 0.09375, ((0, 4),))
    latent_gain = jnp.clip(1.0 + 0.18 * jax.random.normal(splits[9], (LATENT,), jnp.float32), 0.099609375, 1.8984375).astype(jnp.bfloat16)
    absorb_weight = bell_draw(splits[10], (HEADS, QK_NOPE, LATENT), QK_NOPE ** -0.5, 0.5, ((0, 4),))
    value_weight = bell_draw(splits[11], (HEADS, LATENT, VALUE_DIM), LATENT ** -0.5, 0.375, ((0, 4),))
    output_weight = bell_draw(splits[12], (HEADS * VALUE_DIM, D), (HEADS * VALUE_DIM) ** -0.5, 0.125, ((0, 4),))
    mix_gain = jnp.clip(1.0 + 0.18 * jax.random.normal(splits[13], (D,), jnp.float32), 0.099609375, 1.8984375).astype(jnp.bfloat16)
    expert_gain = jnp.clip(1.0 + 0.18 * jax.random.normal(splits[14], (D,), jnp.float32), 0.099609375, 1.8984375).astype(jnp.bfloat16)
    gate_weight = bell_draw(splits[15], (EXPERTS, D, FF), D ** -0.5, 0.09375, ((0, 8), (2, 4)))
    up_weight = bell_draw(splits[16], (EXPERTS, D, FF), D ** -0.5, 0.09375, ((0, 8), (2, 4)))
    down_weight = bell_draw(splits[17], (EXPERTS, FF, D), FF ** -0.5, 0.25, ((0, 8), (1, 4)))
    expert_ids_keys = jax.random.split(jax.random.fold_in(splits[18], 1), BATCH // (SEQ_DEV * N_TP))
    expert_ids_turns = jax.random.permutation(jax.random.fold_in(splits[18], 3), BATCH // (SEQ_DEV * N_TP))
    expert_ids = jax.vmap(lambda own, number: routed_block(jax.random.fold_in(splits[18], 2), own, number, SEQ_DEV * N_TP, EXPERTS, TOPK, CAP, 2))(expert_ids_keys, expert_ids_turns).reshape((BATCH, TOPK))
    route_weights = jnp.clip(0.2 + 0.8 * jax.random.uniform(splits[19], (BATCH, TOPK), jnp.float32) ** level_of(splits[19], (BATCH, TOPK), ((0, 8),), -0.2, 0.2), 0.2, 1.0)
    return {"tokens": tokens, "lengths": lengths, "latent_cache": latent_cache, "rope_cache": rope_cache, "attn_gain": attn_gain, "query_weight": query_weight, "query_rot_weight": query_rot_weight, "latent_weight": latent_weight, "key_rot_weight": key_rot_weight, "latent_gain": latent_gain, "absorb_weight": absorb_weight, "value_weight": value_weight, "output_weight": output_weight, "mix_gain": mix_gain, "expert_gain": expert_gain, "gate_weight": gate_weight, "up_weight": up_weight, "down_weight": down_weight, "expert_ids": expert_ids, "route_weights": route_weights}


norm_floor = 1e-06
rope_base = 10000.0
masked_score = -1e+30
sub_rows = 16

def normed(values, gain):
    wide = values.astype(jnp.float32)
    factor = lax.rsqrt(lax.optimization_barrier(jnp.mean(wide * wide, axis=-1, keepdims=True)) + norm_floor)
    return wide * factor * gain.astype(jnp.float32)

def rotate(values, angle_pos):
    half = values.shape[-1] // 2
    freqs = rope_base ** (-jnp.arange(half, dtype=jnp.float32) / half)
    angles = angle_pos.astype(jnp.float32)[..., None] * freqs
    cosine = jnp.cos(angles)
    sine = jnp.sin(angles)
    first_half = values[..., :half]
    second_half = values[..., half:]
    return jnp.concatenate([first_half * cosine - second_half * sine, second_half * cosine + first_half * sine], axis=-1)

def through_bf16(values):
    return lax.optimization_barrier(values.astype(jnp.bfloat16)).astype(jnp.float32)

def attend_block(operands):
    latents, rotated, query_lat, query_rot, own_lat, own_rot, seq_len = operands
    score_scale = (QK_NOPE + QK_ROPE) ** (-0.5)
    lat_wide = latents.astype(jnp.float32)
    rot_wide = rotated.astype(jnp.float32)
    query_lat = query_lat.astype(jnp.float32)
    query_rot = query_rot.astype(jnp.float32)
    own_lat = own_lat.astype(jnp.float32)
    own_rot = own_rot.astype(jnp.float32)
    scores = (jnp.einsum('bhl,bkl->bhk', query_lat, lat_wide) + jnp.einsum('bhr,bkr->bhk', query_rot, rot_wide)) * score_scale
    valid = jnp.arange(CTX)[None, None, :] < seq_len[:, None, None]
    scores = jnp.where(valid, scores, masked_score)
    own_score = (lax.optimization_barrier(jnp.sum(query_lat * own_lat[:, None, :], axis=-1)) + lax.optimization_barrier(jnp.sum(query_rot * own_rot[:, None, :], axis=-1))) * score_scale
    top = jnp.maximum(lax.optimization_barrier(jnp.max(scores, axis=-1)), own_score)
    weights = jnp.where(valid, jnp.exp(scores - top[..., None]), 0.0)
    own_weight = jnp.exp(own_score - top)
    total = lax.optimization_barrier(jnp.sum(weights, axis=-1)) + own_weight
    summed = jnp.einsum('bhk,bkl->bhl', through_bf16(weights), lat_wide) + through_bf16(own_weight)[..., None] * own_lat[:, None, :]
    return (summed / total[..., None]).astype(jnp.bfloat16)

def reference(tokens, lengths, latent_cache, rope_cache, attn_gain, query_weight, query_rot_weight, latent_weight, key_rot_weight, latent_gain, absorb_weight, value_weight, output_weight, mix_gain, expert_gain, gate_weight, up_weight, down_weight, expert_ids, route_weights):
    batch = tokens.shape[0]
    normed_in = normed(tokens, attn_gain).astype(jnp.bfloat16)
    q_nope = jnp.dot(normed_in, query_weight, preferred_element_type=jnp.float32).astype(jnp.bfloat16)
    q_nope = q_nope.reshape(batch, HEADS, QK_NOPE)
    q_rot = jnp.dot(normed_in, query_rot_weight, preferred_element_type=jnp.float32).reshape(batch, HEADS, QK_ROPE)
    q_rot = rotate(q_rot, lengths[:, None]).astype(jnp.bfloat16)
    q_latent = jnp.einsum('bhn,hnl->bhl', q_nope.astype(jnp.float32), absorb_weight.astype(jnp.float32)).astype(jnp.bfloat16)
    key_raw = jnp.dot(normed_in, jnp.concatenate([latent_weight, key_rot_weight], axis=1), preferred_element_type=jnp.float32)
    new_latent = normed(key_raw[:, :LATENT], latent_gain).astype(jnp.bfloat16)
    new_rope = rotate(key_raw[:, LATENT:], lengths).astype(jnp.bfloat16)
    blocks = batch // 8

    def split_rows(values):
        return values.reshape((blocks, 8) + values.shape[1:])
    head_latent = lax.map(attend_block, (split_rows(latent_cache), split_rows(rope_cache), split_rows(q_latent), split_rows(q_rot), split_rows(new_latent), split_rows(new_rope), split_rows(lengths)))
    head_latent = head_latent.reshape(batch, HEADS, LATENT)
    head_values = jnp.einsum('bhl,hlv->bhv', head_latent.astype(jnp.float32), value_weight.astype(jnp.float32))
    head_values = head_values.astype(jnp.bfloat16).reshape(batch, HEADS * VALUE_DIM)
    group_width = HEADS // N_TP * VALUE_DIM

    def add_group(group, total):
        begin = (group * group_width).astype(jnp.int32)
        columns = lax.dynamic_slice_in_dim(head_values, begin, group_width, 1)
        rows = lax.dynamic_slice_in_dim(output_weight, begin, group_width, 0)
        return total + through_bf16(jnp.dot(columns, rows, preferred_element_type=jnp.float32))
    mixed = lax.fori_loop(0, N_TP, add_group, jnp.zeros((batch, D), jnp.float32)).astype(jnp.bfloat16)
    resid = (tokens.astype(jnp.float32) + normed(mixed, mix_gain)).astype(jnp.bfloat16)
    expert_in = normed(resid, expert_gain).astype(jnp.bfloat16)
    routes = expert_ids.reshape(-1).astype(jnp.int32)
    count_routes = routes.shape[0]
    order = jnp.argsort(routes, stable=True).astype(jnp.int32)
    picks = (routes[:, None] == jnp.arange(EXPERTS, dtype=jnp.int32)[None, :]).astype(jnp.int32)
    loads = lax.optimization_barrier(jnp.sum(picks, axis=0)).astype(jnp.int32)
    offsets = (jnp.cumsum(loads) - loads).astype(jnp.int32)
    inverse = jnp.zeros((count_routes,), jnp.int32).at[order].set(jnp.arange(count_routes, dtype=jnp.int32))
    most_rows = N_EP * CAP
    padded = jnp.concatenate([order, jnp.zeros((most_rows,), jnp.int32)])
    ff_group = FF // N_TP

    def run_expert(operands):
        gate_mat, up_mat, down_mat, begin, load = operands
        chosen = lax.dynamic_slice_in_dim(padded, begin.astype(jnp.int32), most_rows, 0)
        rows_all = expert_in[chosen // TOPK]

        def compute(rows_in):
            gate = jnp.dot(rows_in, gate_mat, preferred_element_type=jnp.float32)
            upward = jnp.dot(rows_in, up_mat, preferred_element_type=jnp.float32)
            hidden = (jax.nn.silu(gate) * upward).astype(jnp.bfloat16)
            parts = jnp.einsum('rgf,gfd->rgd', hidden.reshape(sub_rows, N_TP, ff_group).astype(jnp.float32), down_mat.reshape(N_TP, ff_group, D).astype(jnp.float32))
            return lax.optimization_barrier(jnp.sum(through_bf16(parts), axis=1)).astype(jnp.bfloat16)

        def empty_rows(rows_in):
            return jnp.zeros((sub_rows, D), jnp.bfloat16)
        pieces = []
        for piece_index in range(most_rows // sub_rows):
            rows = rows_all[piece_index * sub_rows:(piece_index + 1) * sub_rows]
            pieces.append(lax.cond(piece_index * sub_rows < load, compute, empty_rows, rows))
        return jnp.concatenate(pieces, axis=0)
    results = lax.map(run_expert, (gate_weight, up_weight, down_weight, offsets, loads))
    ranks = inverse - offsets[routes]
    picked = results.reshape(EXPERTS * most_rows, D)[routes * most_rows + ranks]
    moe_out = lax.optimization_barrier(jnp.sum(picked.astype(jnp.float32).reshape(batch, TOPK, D) * route_weights[:, :, None], axis=1))
    out = (resid.astype(jnp.float32) + moe_out).astype(jnp.bfloat16)
    return (out, new_latent, new_rope)
```

```python
import functools

import jax
import jax.numpy as jnp
from jax import lax
from jax.experimental import pallas as pl
from jax.experimental.pallas import tpu as pltpu
from jax.sharding import PartitionSpec as P

norm_floor = 1e-06
rope_base = 10000.0
masked_score = -1e30
MESH = pl.DeviceIdType.MESH
F32 = jnp.float32
BF16 = jnp.bfloat16


def dot(a, b):
    return jnp.dot(a, b, preferred_element_type=F32)


def dot_nt(a, b):
    return lax.dot_general(a, b, (((1,), (1,)), ((), ())), preferred_element_type=F32)


def rounded(v):
    return v.astype(BF16).astype(F32)


def norm_rows(wide, gain):
    factor = lax.rsqrt(jnp.mean(wide * wide, axis=-1, keepdims=True) + norm_floor)
    return wide * factor * gain.astype(F32)


def body(
    E, T, CAP,
    tokens, lengths, cos_ref, sin_ref, attn_gain, latent_gain, mix_gain, expert_gain, ids, rw,
    h_qw, h_qr, h_lw, h_kr, h_ab, h_lat, h_rope, h_vw, h_ow, h_gw, h_uw, h_dw,
    out, new_latent, new_rope,
    qw, qr, lw, kr, ab, lat, rope, vw, ow, gw, uw, dw,
    recv1, xs, nin, send2, recv2, qs, send3, recv3, hl, send4, recv4, resid, send5, recv5, xe,
    send6, recv6, ys,
    lsem, s1, r1, s2, r2, s3, r3, s4, r4, s5, r5, s6, r6,
):
    ep = lax.axis_index("ep")
    tp = lax.axis_index("tp")
    N = E * T
    me = ep * T + tp
    R, D = tokens.shape
    G = R * T
    Hd, NOPE, LAT = ab.shape
    ROT = kr.shape[1]
    half = ROT // 2
    scale = (NOPE + ROT) ** (-0.5)
    cw = D // T
    slots = E * CAP

    pairs = [
        (h_lw, lw), (h_kr, kr), (h_qw, qw), (h_qr, qr), (h_ab, ab), (h_lat, lat), (h_rope, rope),
        (h_vw, vw), (h_ow, ow), (h_gw, gw), (h_uw, uw), (h_dw, dw),
    ]
    loads = [pltpu.make_async_copy(a, b, lsem.at[i]) for i, (a, b) in enumerate(pairs)]
    for c in loads:
        c.start()
    c_lw, c_kr, c_qw, c_qr, c_ab, c_lat, c_rope, c_vw, c_ow, c_gw, c_uw, c_dw = loads

    barrier = pltpu.get_barrier_semaphore()

    def greet(d, carry):
        other = lax.rem(me + d, N)
        pl.semaphore_signal(
            barrier, inc=1, device_id=(other // T, lax.rem(other, T)), device_id_type=MESH
        )
        return carry

    lax.fori_loop(1, N, greet, 0)
    pl.semaphore_wait(barrier, N - 1)

    def tp_copy(d, src, dst, ss, rs):
        return pltpu.make_async_remote_copy(
            src_ref=src, dst_ref=dst, send_sem=ss, recv_sem=rs,
            device_id=(ep, lax.rem(tp + d, T)), device_id_type=MESH,
        )

    c1 = [tp_copy(d, tokens, recv1.at[tp], s1.at[d], r1.at[d]) for d in range(1, T)]
    for c in c1:
        c.start()
    recv1[tp] = tokens[...]
    idv = ids[...]
    lane_e = lax.broadcasted_iota(jnp.int32, (G, E), 1)
    topk = idv.shape[1]
    hits = [(idv[:, k:k + 1] == lane_e).astype(F32) for k in range(topk)]
    named = sum(hits)
    lower = (
        lax.broadcasted_iota(jnp.int32, (G, G), 1) < lax.broadcasted_iota(jnp.int32, (G, G), 0)
    ).astype(F32)
    before = dot(lower.astype(BF16), named.astype(BF16))
    lane_s = lax.broadcasted_iota(jnp.int32, (G, slots), 1)
    row_s = lax.broadcasted_iota(jnp.int32, (slots, G), 0)
    lane0 = (lax.broadcasted_iota(jnp.int32, (slots, 128), 1) == 0).astype(BF16)
    picks = []
    spread = jnp.zeros((slots, G), F32)
    for k in range(topk):
        rank = jnp.sum(hits[k] * before, axis=1, keepdims=True)
        target = idv[:, k:k + 1].astype(F32) * CAP + rank
        picks.append((target.astype(jnp.int32) == lane_s).astype(F32).astype(BF16))
        across = dot_nt(lane0, jnp.broadcast_to(target, (G, 128)).astype(BF16))
        spread = spread + (across.astype(jnp.int32) == row_s).astype(F32)
    spread = spread.astype(BF16)
    send2[...] = jnp.zeros_like(send2)
    for c in c1:
        c.wait()
    for t in range(T):
        xs[t * R:(t + 1) * R, :] = recv1[t].astype(F32)
    nin[...] = norm_rows(xs[...], attn_gain[...]).astype(BF16)

    c_lw.wait()
    c_kr.wait()
    kd = lw.shape[0]
    mine = nin[:, pl.ds(pl.multiple_of(tp * kd, kd), kd)]
    k_lat = dot(mine, lw[...])
    k_rot = dot(mine, kr[...])
    for b in range(G):
        send2[b // R, b % R, Hd:Hd + 1, 0:LAT] = k_lat[b:b + 1]
        send2[b // R, b % R, Hd:Hd + 1, LAT:LAT + ROT] = k_rot[b:b + 1]
    c_qr.wait()
    q_rot = dot(nin[...], qr[...])
    cosv = cos_ref[...]
    sinv = sin_ref[...]
    for h in range(Hd):
        a = q_rot[:, h * ROT:h * ROT + half]
        b2 = q_rot[:, h * ROT + half:(h + 1) * ROT]
        ra = rounded(a * cosv - b2 * sinv)
        rb = rounded(b2 * cosv + a * sinv)
        for b in range(G):
            send2[b // R, b % R, h:h + 1, LAT:LAT + half] = ra[b:b + 1]
            send2[b // R, b % R, h:h + 1, LAT + half:LAT + ROT] = rb[b:b + 1]
    c_qw.wait()
    c_ab.wait()
    for h in range(Hd):
        q = dot(nin[...], qw[:, h * NOPE:(h + 1) * NOPE]).astype(BF16)
        ql = rounded(dot(q, ab[h]))
        for b in range(G):
            send2[b // R, b % R, h:h + 1, 0:LAT] = ql[b:b + 1]
    c2 = [
        tp_copy(d, send2.at[lax.rem(tp + d, T)], recv2.at[tp], s2.at[d], r2.at[d])
        for d in range(1, T)
    ]
    for c in c2:
        c.start()
    recv2[tp] = send2[tp]
    for c in c2:
        c.wait()

    c_lat.wait()
    c_rope.wait()
    for s in range(R):
        raw = sum(recv2[t, s, Hd:Hd + 1, :] for t in range(T))
        nl = norm_rows(raw[:, 0:LAT], latent_gain[...]).astype(BF16)
        cs = cos_ref[pl.ds(tp * R + s, 1), :]
        sn = sin_ref[pl.ds(tp * R + s, 1), :]
        a = raw[:, LAT:LAT + half]
        b2 = raw[:, LAT + half:LAT + ROT]
        nr = jnp.concatenate([a * cs - b2 * sn, b2 * cs + a * sn], axis=1).astype(BF16)
        new_latent[s:s + 1, :] = nl
        new_rope[s:s + 1, :] = nr
        nl = nl.astype(F32)
        nr = nr.astype(F32)
        for t in range(T):
            qs[s, t * Hd:(t + 1) * Hd, :] = recv2[t, s, 0:Hd, :]
        q_l = qs[s, :, 0:LAT]
        q_r = qs[s, :, LAT:LAT + ROT]
        own = (
            jnp.sum(q_l * nl, axis=1, keepdims=True) + jnp.sum(q_r * nr, axis=1, keepdims=True)
        ) * scale
        sc = (dot_nt(q_l.astype(BF16), lat[s]) + dot_nt(q_r.astype(BF16), rope[s])) * scale
        valid = lax.broadcasted_iota(jnp.int32, sc.shape, 1) < lengths[tp * R + s]
        sc = jnp.where(valid, sc, masked_score)
        top = jnp.maximum(jnp.max(sc, axis=1, keepdims=True), own)
        w = jnp.where(valid, jnp.exp(sc - top), 0.0)
        ow_ = jnp.exp(own - top)
        total = jnp.sum(w, axis=1, keepdims=True) + ow_
        o = rounded((dot(w.astype(BF16), lat[s]) + rounded(ow_) * nl) / total)
        for t in range(T):
            for h in range(Hd):
                send3[t, h, s:s + 1, :] = o[t * Hd + h:t * Hd + h + 1]
    c3 = [
        tp_copy(d, send3.at[lax.rem(tp + d, T)], recv3.at[tp], s3.at[d], r3.at[d])
        for d in range(1, T)
    ]
    for c in c3:
        c.start()
    recv3[tp] = send3[tp]
    c_vw.wait()
    c_ow.wait()
    for c in c3:
        c.wait()

    for h in range(Hd):
        for t in range(T):
            hl[h, t * R:(t + 1) * R, :] = recv3[t, h]
    hv = jnp.concatenate(
        [dot(hl[h].astype(BF16), vw[h]).astype(BF16) for h in range(Hd)], axis=1
    )
    c4 = []
    for j in range(T):
        part = dot(hv, ow[:, j * cw:(j + 1) * cw]).astype(BF16)
        send4[j] = part
        recv4[j, tp] = part
        for d in range(1, T):
            c = tp_copy(d, send4.at[j], recv4.at[j, tp], s4.at[j, d], r4.at[j, d])
            c.start()
            c4.append(c)
    for c in c4:
        c.wait()
    for j in range(T):
        total = sum(recv4[j, t].astype(F32) for t in range(T))
        resid[:, j * cw:(j + 1) * cw] = rounded(total)
    res = rounded(xs[...] + norm_rows(resid[...], mix_gain[...]))
    resid[...] = res
    e_in = norm_rows(res, expert_gain[...]).astype(BF16)

    outgoing = dot(spread, e_in)
    for e in range(E):
        send5[e] = outgoing[e * CAP:(e + 1) * CAP].astype(BF16)
    c5 = []
    for d in range(1, E):
        other = lax.rem(ep + d, E)
        c = pltpu.make_async_remote_copy(
            src_ref=send5.at[other], dst_ref=recv5.at[ep], send_sem=s5.at[d], recv_sem=r5.at[d],
            device_id=(other, tp), device_id_type=MESH,
        )
        c.start()
        c5.append(c)
    recv5[ep] = send5[ep]
    c_gw.wait()
    c_uw.wait()
    c_dw.wait()
    for c in c5:
        c.wait()
    for e in range(E):
        xe[e * CAP:(e + 1) * CAP, :] = recv5[e].astype(F32)
    x = xe[...].astype(BF16)
    gate = dot(x, gw[0])
    upward = dot(x, uw[0])
    hidden = (gate / (1.0 + jnp.exp(-gate)) * upward).astype(BF16)
    for j in range(T):
        part = dot(hidden, dw[0, :, j * cw:(j + 1) * cw])
        for e in range(E):
            send6[e * T + j] = part[e * CAP:(e + 1) * CAP].astype(BF16)

    def back(d):
        other = lax.rem(me + d, N)
        return pltpu.make_async_remote_copy(
            src_ref=send6.at[other], dst_ref=recv6.at[me], send_sem=s6.at[d], recv_sem=r6.at[d],
            device_id=(other // T, lax.rem(other, T)), device_id_type=MESH,
        )

    def go(d, carry):
        back(d).start()
        return carry

    def come(d, carry):
        back(d).wait()
        return carry

    lax.fori_loop(1, N, go, 0)
    recv6[me] = send6[me]
    lax.fori_loop(1, N, come, 0)
    for e in range(E):
        ys[e * CAP:(e + 1) * CAP, :] = sum(recv6[e * T + t].astype(F32) for t in range(T))
    y = ys[...].astype(BF16)
    acc = resid[:, pl.ds(pl.multiple_of(tp * cw, cw), cw)]
    add = sum(dot(picks[k], y) * rw[:, k:k + 1] for k in range(topk))
    out[...] = (acc + add).astype(BF16)


def per_device(
    tokens, lengths, latent_cache, rope_cache, attn_gain, query_weight, query_rot_weight,
    latent_weight, key_rot_weight, latent_gain, absorb_weight, value_weight, output_weight,
    mix_gain, expert_gain, gate_weight, up_weight, down_weight, expert_ids, route_weights,
):
    E = lax.axis_size("ep")
    T = lax.axis_size("tp")
    R, D = tokens.shape
    G = R * T
    Hd, NOPE, LAT = absorb_weight.shape
    H = Hd * T
    ROT = key_rot_weight.shape[1]
    CAP = 2 * expert_ids.shape[0] * expert_ids.shape[1] // E
    cw = D // T
    half = ROT // 2
    wq = LAT + -(-ROT // 128) * 128
    freqs = rope_base ** (-jnp.arange(half, dtype=F32) / half)
    angles = lengths.astype(F32)[:, None] * freqs
    weights = (
        query_weight, query_rot_weight, latent_weight, key_rot_weight, absorb_weight,
        latent_cache, rope_cache, value_weight, output_weight, gate_weight, up_weight, down_weight,
    )
    vm = pl.BlockSpec(memory_space=pltpu.VMEM)
    sm = pl.BlockSpec(memory_space=pltpu.SMEM)
    anyw = pl.BlockSpec(memory_space=pl.ANY)
    dma = pltpu.SemaphoreType.DMA
    N = E * T
    return pl.pallas_call(
        functools.partial(body, E, T, CAP),
        out_shape=(
            jax.ShapeDtypeStruct((G, cw), BF16),
            jax.ShapeDtypeStruct((R, LAT), BF16),
            jax.ShapeDtypeStruct((R, ROT), BF16),
        ),
        in_specs=[vm, sm] + [vm] * 8 + [anyw] * 12,
        out_specs=(vm, vm, vm),
        scratch_shapes=[pltpu.VMEM(w.shape, w.dtype) for w in weights]
        + [
            pltpu.VMEM((T, R, D), BF16),
            pltpu.VMEM((G, D), F32),
            pltpu.VMEM((G, D), BF16),
            pltpu.VMEM((T, R, Hd + 1, wq), F32),
            pltpu.VMEM((T, R, Hd + 1, wq), F32),
            pltpu.VMEM((R, H, wq), F32),
            pltpu.VMEM((T, Hd, R, LAT), F32),
            pltpu.VMEM((T, Hd, R, LAT), F32),
            pltpu.VMEM((Hd, G, LAT), F32),
            pltpu.VMEM((T, G, cw), BF16),
            pltpu.VMEM((T, T, G, cw), BF16),
            pltpu.VMEM((G, D), F32),
            pltpu.VMEM((E, CAP, D), BF16),
            pltpu.VMEM((E, CAP, D), BF16),
            pltpu.VMEM((E * CAP, D), F32),
            pltpu.VMEM((N, CAP, cw), BF16),
            pltpu.VMEM((N, CAP, cw), BF16),
            pltpu.VMEM((E * CAP, cw), F32),
            dma((12,)),
            dma((T,)), dma((T,)), dma((T,)), dma((T,)), dma((T,)), dma((T,)),
            dma((T, T)), dma((T, T)), dma((E,)), dma((E,)), dma((N,)), dma((N,)),
        ],
        compiler_params=pltpu.CompilerParams(
            collective_id=0, has_side_effects=True, vmem_limit_bytes=48 * 1024 * 1024
        ),
    )(
        tokens, lengths, jnp.cos(angles), jnp.sin(angles), attn_gain[None], latent_gain[None],
        mix_gain[None], expert_gain[None], expert_ids, route_weights, *weights,
    )


def solution(mesh):
    placed = (
        P(("ep", "tp"), None), P("ep"), P(("ep", "tp"), None, None), P(("ep", "tp"), None, None),
        P(), P(None, "tp"), P(None, "tp"), P("tp", None), P("tp", None), P(),
        P("tp", None, None), P("tp", None, None), P("tp", None), P(), P(),
        P("ep", None, "tp"), P("ep", None, "tp"), P("ep", "tp", None), P("ep", None), P("ep", None),
    )
    return jax.shard_map(
        per_device,
        mesh=mesh,
        in_specs=placed,
        out_specs=(P("ep", "tp"), P(("ep", "tp"), None), P(("ep", "tp"), None)),
        check_vma=False,
    )
```

```python
import functools

import jax
import jax.numpy as jnp
import numpy as np
from jax import lax
from jax.experimental import pallas as pl
from jax.experimental.pallas import tpu as pltpu
from jax.sharding import PartitionSpec as P

norm_floor = 1e-06
rope_base = 10000.0
masked_score = -1e30
turn_high = 6.28125
turn_low = 2 * np.pi - 6.28125
MESH = pl.DeviceIdType.MESH
F32 = jnp.float32
BF16 = jnp.bfloat16


def dot(a, b):
    return jnp.dot(a, b, preferred_element_type=F32)


def dot_nt(a, b):
    return lax.dot_general(a, b, (((1,), (1,)), ((), ())), preferred_element_type=F32)


def rounded(v):
    return v.astype(BF16).astype(F32)


def fold(gain):
    return gain.reshape(-1, 128)


def norm_rows(wide, gain):
    factor = lax.rsqrt(jnp.mean(wide * wide, axis=-1, keepdims=True) + norm_floor)
    return wide * factor * gain.astype(F32)


def body(
    E, T, CAP,
    tokens, lengths, freqs, g_attn, g_lat, g_mix, g_expert, ids, rw,
    h_qw, h_qr, h_lw, h_kr, h_ab, h_lat, h_rope, h_vw, h_ow, h_gw, h_uw, h_dw,
    out, new_latent, new_rope,
    qw, qr, lw, kr, ab, lat, rope, vw, ow, gw, uw, dw,
    recv1, xs, nin, send2, recv2, qs, send3, recv3, hl, send4, recv4, resid, send5, recv5, xe,
    send6, recv6, ys,
    cos_ref, sin_ref, attn_gain, latent_gain, mix_gain, expert_gain,
    lsem, s1, r1, s2, r2, s3, r3, s4, r4, s5, r5, s6, r6,
):
    ep = lax.axis_index("ep")
    tp = lax.axis_index("tp")
    N = E * T
    me = ep * T + tp
    R, D = tokens.shape
    G = R * T
    Hd, NOPE, LAT = ab.shape
    ROT = kr.shape[0]
    half = ROT // 2
    scale = (NOPE + ROT) ** (-0.5)
    cw = D // T
    slots = E * CAP

    pairs = [
        (h_lw, lw), (h_kr, kr), (h_qw, qw), (h_qr, qr), (h_ab, ab), (h_lat, lat), (h_rope, rope),
        (h_vw, vw), (h_ow, ow), (h_gw, gw), (h_uw, uw), (h_dw, dw),
    ]
    loads = [pltpu.make_async_copy(a, b, lsem.at[i]) for i, (a, b) in enumerate(pairs)]
    for c in loads:
        c.start()
    c_lw, c_kr, c_qw, c_qr, c_ab, c_lat, c_rope, c_vw, c_ow, c_gw, c_uw, c_dw = loads

    barrier = pltpu.get_barrier_semaphore()

    def greet(d, carry):
        other = lax.rem(me + d, N)
        pl.semaphore_signal(
            barrier, inc=1, device_id=(other // T, lax.rem(other, T)), device_id_type=MESH
        )
        return carry

    lax.fori_loop(1, N, greet, 0)
    pl.semaphore_wait(barrier, N - 1)

    def tp_copy(d, src, dst, ss, rs):
        return pltpu.make_async_remote_copy(
            src_ref=src, dst_ref=dst, send_sem=ss, recv_sem=rs,
            device_id=(ep, lax.rem(tp + d, T)), device_id_type=MESH,
        )

    c1 = [tp_copy(d, tokens, recv1.at[tp], s1.at[d], r1.at[d]) for d in range(1, T)]
    for c in c1:
        c.start()
    recv1[tp] = tokens[...]
    for src, dst in (
        (g_attn, attn_gain), (g_lat, latent_gain), (g_mix, mix_gain), (g_expert, expert_gain)
    ):
        rows = src[...].astype(F32)
        for i in range(src.shape[0]):
            wide = src.shape[1]
            dst[:, i * wide:(i + 1) * wide] = rows[i:i + 1]
    row_g = lax.broadcasted_iota(jnp.int32, (G, 1), 0)
    pos = jnp.zeros((G, 1), F32)
    for b in range(G):
        pos = jnp.where(row_g == b, lengths[b].astype(F32), pos)
    angles = pos * freqs[...]
    turns = jnp.floor(angles * (0.5 / np.pi) + 0.5)
    angles = (angles - turns * turn_high) - turns * turn_low
    cos_ref[...] = jnp.cos(angles)
    sin_ref[...] = jnp.sin(angles)
    eye = (
        lax.broadcasted_iota(jnp.int32, (G, G), 1) == lax.broadcasted_iota(jnp.int32, (G, G), 0)
    ).astype(F32)
    topk = ids.shape[0]

    def column(row):
        return jnp.sum(eye * row, axis=1, keepdims=True)

    ide = [column(ids[k:k + 1, :].astype(F32)) for k in range(topk)]
    rwe = [column(rw[k:k + 1, :]) for k in range(topk)]
    lane_e = lax.broadcasted_iota(jnp.int32, (G, E), 1).astype(F32)
    hits = [(ide[k] == lane_e).astype(F32) for k in range(topk)]
    named = sum(hits)
    lower = (
        lax.broadcasted_iota(jnp.int32, (G, G), 1) < lax.broadcasted_iota(jnp.int32, (G, G), 0)
    ).astype(F32)
    before = dot(lower.astype(BF16), named.astype(BF16))
    lane_s = lax.broadcasted_iota(jnp.int32, (G, slots), 1)
    row_s = lax.broadcasted_iota(jnp.int32, (slots, G), 0)
    lane0 = (lax.broadcasted_iota(jnp.int32, (slots, 128), 1) == 0).astype(BF16)
    picks = []
    spread = jnp.zeros((slots, G), F32)
    for k in range(topk):
        rank = jnp.sum(hits[k] * before, axis=1, keepdims=True)
        target = ide[k] * CAP + rank
        picks.append((target.astype(jnp.int32) == lane_s).astype(F32).astype(BF16))
        across = dot_nt(lane0, jnp.broadcast_to(target, (G, 128)).astype(BF16))
        spread = spread + (across.astype(jnp.int32) == row_s).astype(F32)
    spread = spread.astype(BF16)
    send2[...] = jnp.zeros_like(send2)
    for c in c1:
        c.wait()
    for t in range(T):
        xs[t * R:(t + 1) * R, :] = recv1[t].astype(F32)
    nin[...] = norm_rows(xs[...], attn_gain[...]).astype(BF16)

    c_lw.wait()
    c_kr.wait()
    kd = lw.shape[0]
    mine = nin[:, pl.ds(pl.multiple_of(tp * kd, kd), kd)]
    k_lat = dot(mine, lw[...])
    k_rot = dot_nt(mine, kr[...])
    for b in range(G):
        send2[b // R, b % R, Hd:Hd + 1, 0:LAT] = k_lat[b:b + 1]
        send2[b // R, b % R, Hd:Hd + 1, LAT:LAT + ROT] = k_rot[b:b + 1]
    c_qr.wait()
    q_rot = dot(nin[...], qr[...])
    cosv = cos_ref[...]
    sinv = sin_ref[...]
    for h in range(Hd):
        a = q_rot[:, h * ROT:h * ROT + half]
        b2 = q_rot[:, h * ROT + half:(h + 1) * ROT]
        ra = rounded(a * cosv - b2 * sinv)
        rb = rounded(b2 * cosv + a * sinv)
        for b in range(G):
            send2[b // R, b % R, h:h + 1, LAT:LAT + half] = ra[b:b + 1]
            send2[b // R, b % R, h:h + 1, LAT + half:LAT + ROT] = rb[b:b + 1]
    c_qw.wait()
    c_ab.wait()
    for h in range(Hd):
        q = dot(nin[...], qw[:, h * NOPE:(h + 1) * NOPE]).astype(BF16)
        ql = rounded(dot(q, ab[h]))
        for b in range(G):
            send2[b // R, b % R, h:h + 1, 0:LAT] = ql[b:b + 1]
    c2 = [
        tp_copy(d, send2.at[lax.rem(tp + d, T)], recv2.at[tp], s2.at[d], r2.at[d])
        for d in range(1, T)
    ]
    for c in c2:
        c.start()
    recv2[tp] = send2[tp]
    for c in c2:
        c.wait()

    c_lat.wait()
    c_rope.wait()
    for s in range(R):
        raw = sum(recv2[t, s, Hd:Hd + 1, :] for t in range(T))
        nl = norm_rows(raw[:, 0:LAT], latent_gain[...]).astype(BF16)
        cs = cos_ref[pl.ds(tp * R + s, 1), :]
        sn = sin_ref[pl.ds(tp * R + s, 1), :]
        a = raw[:, LAT:LAT + half]
        b2 = raw[:, LAT + half:LAT + ROT]
        nr = jnp.concatenate([a * cs - b2 * sn, b2 * cs + a * sn], axis=1).astype(BF16)
        new_latent[s:s + 1, :] = nl
        new_rope[s:s + 1, :] = nr
        nl = nl.astype(F32)
        nr = nr.astype(F32)
        for t in range(T):
            qs[s, t * Hd:(t + 1) * Hd, :] = recv2[t, s, 0:Hd, :]
        q_l = qs[s, :, 0:LAT]
        q_r = qs[s, :, LAT:LAT + ROT]
        own = (
            jnp.sum(q_l * nl, axis=1, keepdims=True) + jnp.sum(q_r * nr, axis=1, keepdims=True)
        ) * scale
        sc = (dot_nt(q_l.astype(BF16), lat[s]) + dot(q_r.astype(BF16), rope[s])) * scale
        valid = lax.broadcasted_iota(jnp.int32, sc.shape, 1) < lengths[tp * R + s]
        sc = jnp.where(valid, sc, masked_score)
        top = jnp.maximum(jnp.max(sc, axis=1, keepdims=True), own)
        w = jnp.where(valid, jnp.exp(sc - top), 0.0)
        ow_ = jnp.exp(own - top)
        total = jnp.sum(w, axis=1, keepdims=True) + ow_
        o = rounded((dot(w.astype(BF16), lat[s]) + rounded(ow_) * nl) / total)
        for t in range(T):
            for h in range(Hd):
                send3[t, h, s:s + 1, :] = o[t * Hd + h:t * Hd + h + 1]
    c3 = [
        tp_copy(d, send3.at[lax.rem(tp + d, T)], recv3.at[tp], s3.at[d], r3.at[d])
        for d in range(1, T)
    ]
    for c in c3:
        c.start()
    recv3[tp] = send3[tp]
    c_vw.wait()
    c_ow.wait()
    for c in c3:
        c.wait()

    for h in range(Hd):
        for t in range(T):
            hl[h, t * R:(t + 1) * R, :] = recv3[t, h]
    hv = jnp.concatenate(
        [dot(hl[h].astype(BF16), vw[h]).astype(BF16) for h in range(Hd)], axis=1
    )
    c4 = []
    for j in range(T):
        part = dot(hv, ow[:, j * cw:(j + 1) * cw]).astype(BF16)
        send4[j] = part
        recv4[j, tp] = part
        for d in range(1, T):
            c = tp_copy(d, send4.at[j], recv4.at[j, tp], s4.at[j, d], r4.at[j, d])
            c.start()
            c4.append(c)
    for c in c4:
        c.wait()
    for j in range(T):
        total = sum(recv4[j, t].astype(F32) for t in range(T))
        resid[:, j * cw:(j + 1) * cw] = rounded(total)
    res = rounded(xs[...] + norm_rows(resid[...], mix_gain[...]))
    resid[...] = res
    e_in = norm_rows(res, expert_gain[...]).astype(BF16)

    outgoing = dot(spread, e_in)
    for e in range(E):
        send5[e] = outgoing[e * CAP:(e + 1) * CAP].astype(BF16)
    c5 = []
    for d in range(1, E):
        other = lax.rem(ep + d, E)
        c = pltpu.make_async_remote_copy(
            src_ref=send5.at[other], dst_ref=recv5.at[ep], send_sem=s5.at[d], recv_sem=r5.at[d],
            device_id=(other, tp), device_id_type=MESH,
        )
        c.start()
        c5.append(c)
    recv5[ep] = send5[ep]
    c_gw.wait()
    c_uw.wait()
    c_dw.wait()
    for c in c5:
        c.wait()
    for e in range(E):
        xe[e * CAP:(e + 1) * CAP, :] = recv5[e].astype(F32)
    x = xe[...].astype(BF16)
    gate = dot(x, gw[0])
    upward = dot(x, uw[0])
    hidden = (gate / (1.0 + jnp.exp(-gate)) * upward).astype(BF16)
    for j in range(T):
        part = dot(hidden, dw[0, :, j * cw:(j + 1) * cw])
        for e in range(E):
            send6[e * T + j] = part[e * CAP:(e + 1) * CAP].astype(BF16)

    def back(d):
        other = lax.rem(me + d, N)
        return pltpu.make_async_remote_copy(
            src_ref=send6.at[other], dst_ref=recv6.at[me], send_sem=s6.at[d], recv_sem=r6.at[d],
            device_id=(other // T, lax.rem(other, T)), device_id_type=MESH,
        )

    def go(d, carry):
        back(d).start()
        return carry

    def come(d, carry):
        back(d).wait()
        return carry

    lax.fori_loop(1, N, go, 0)
    recv6[me] = send6[me]
    lax.fori_loop(1, N, come, 0)
    for e in range(E):
        ys[e * CAP:(e + 1) * CAP, :] = sum(recv6[e * T + t].astype(F32) for t in range(T))
    y = ys[...].astype(BF16)
    acc = resid[:, pl.ds(pl.multiple_of(tp * cw, cw), cw)]
    add = sum(dot(picks[k], y) * rwe[k] for k in range(topk))
    out[...] = (acc + add).astype(BF16)


def per_device(
    tokens, lengths, latent_cache, rope_cache, attn_gain, query_weight, query_rot_weight,
    latent_weight, key_rot_weight, latent_gain, absorb_weight, value_weight, output_weight,
    mix_gain, expert_gain, gate_weight, up_weight, down_weight, expert_ids, route_weights,
):
    E = lax.axis_size("ep")
    T = lax.axis_size("tp")
    R, D = tokens.shape
    G = R * T
    Hd, NOPE, LAT = absorb_weight.shape
    H = Hd * T
    ROT = key_rot_weight.shape[1]
    CAP = 2 * expert_ids.shape[0] * expert_ids.shape[1] // E
    cw = D // T
    half = ROT // 2
    wq = LAT + -(-ROT // 128) * 128
    freqs = jnp.asarray(rope_base ** (-np.arange(half) / half), F32)[None]
    key_rot_t = key_rot_weight.T
    rope_t = jnp.swapaxes(rope_cache, 1, 2)
    weights = (
        query_weight, query_rot_weight, latent_weight, key_rot_t, absorb_weight,
        latent_cache, rope_t, value_weight, output_weight, gate_weight, up_weight, down_weight,
    )
    vm = pl.BlockSpec(memory_space=pltpu.VMEM)
    sm = pl.BlockSpec(memory_space=pltpu.SMEM)
    anyw = pl.BlockSpec(memory_space=pltpu.HBM)
    dma = pltpu.SemaphoreType.DMA
    N = E * T
    return pl.pallas_call(
        functools.partial(body, E, T, CAP),
        out_shape=(
            jax.ShapeDtypeStruct((G, cw), BF16),
            jax.ShapeDtypeStruct((R, LAT), BF16),
            jax.ShapeDtypeStruct((R, ROT), BF16),
        ),
        in_specs=[vm, sm] + [vm] * 7 + [anyw] * 12,
        out_specs=(vm, vm, vm),
        scratch_shapes=[pltpu.VMEM(w.shape, w.dtype) for w in weights]
        + [
            pltpu.VMEM((T, R, D), BF16),
            pltpu.VMEM((G, D), F32),
            pltpu.VMEM((G, D), BF16),
            pltpu.VMEM((T, R, Hd + 1, wq), F32),
            pltpu.VMEM((T, R, Hd + 1, wq), F32),
            pltpu.VMEM((R, H, wq), F32),
            pltpu.VMEM((T, Hd, R, LAT), F32),
            pltpu.VMEM((T, Hd, R, LAT), F32),
            pltpu.VMEM((Hd, G, LAT), F32),
            pltpu.VMEM((T, G, cw), BF16),
            pltpu.VMEM((T, T, G, cw), BF16),
            pltpu.VMEM((G, D), F32),
            pltpu.VMEM((E, CAP, D), BF16),
            pltpu.VMEM((E, CAP, D), BF16),
            pltpu.VMEM((E * CAP, D), F32),
            pltpu.VMEM((N, CAP, cw), BF16),
            pltpu.VMEM((N, CAP, cw), BF16),
            pltpu.VMEM((E * CAP, cw), F32),
            pltpu.VMEM((G, half), F32),
            pltpu.VMEM((G, half), F32),
            pltpu.VMEM((1, D), F32),
            pltpu.VMEM((1, LAT), F32),
            pltpu.VMEM((1, D), F32),
            pltpu.VMEM((1, D), F32),
            dma((12,)),
            dma((T,)), dma((T,)), dma((T,)), dma((T,)), dma((T,)), dma((T,)),
            dma((T, T)), dma((T, T)), dma((E,)), dma((E,)), dma((N,)), dma((N,)),
        ],
        compiler_params=pltpu.CompilerParams(
            collective_id=0, has_side_effects=True, vmem_limit_bytes=63 * 1024 * 1024
        ),
    )(
        tokens, lengths, freqs, fold(attn_gain), fold(latent_gain), fold(mix_gain),
        fold(expert_gain), expert_ids.T, route_weights.T, *weights,
    )


def solution(mesh):
    placed = (
        P(("ep", "tp"), None), P("ep"), P(("ep", "tp"), None, None), P(("ep", "tp"), None, None),
        P(), P(None, "tp"), P(None, "tp"), P("tp", None), P("tp", None), P(),
        P("tp", None, None), P("tp", None, None), P("tp", None), P(), P(),
        P("ep", None, "tp"), P("ep", None, "tp"), P("ep", "tp", None), P("ep", None), P("ep", None),
    )
    return jax.shard_map(
        per_device,
        mesh=mesh,
        in_specs=placed,
        out_specs=(P("ep", "tp"), P(("ep", "tp"), None), P(("ep", "tp"), None)),
        check_vma=False,
    )
```

```python
import functools

import jax
import jax.numpy as jnp
import numpy as np
from jax import lax
from jax.experimental import pallas as pl
from jax.experimental.pallas import tpu as pltpu
from jax.sharding import PartitionSpec as P

norm_floor = 1e-06
rope_base = 10000.0
masked_score = -1e30
turn_high = 6.28125
turn_low = 2 * np.pi - 6.28125
MESH = pl.DeviceIdType.MESH
F32 = jnp.float32
BF16 = jnp.bfloat16


def dot(a, b):
    return jnp.dot(a, b, preferred_element_type=F32)


def dot_nt(a, b):
    return lax.dot_general(a, b, (((1,), (1,)), ((), ())), preferred_element_type=F32)


def rounded(v):
    return v.astype(BF16).astype(F32)


def fold(gain):
    return gain.reshape(-1, 128)


def norm_rows(wide, gain):
    factor = lax.rsqrt(jnp.mean(wide * wide, axis=-1, keepdims=True) + norm_floor)
    return wide * factor * gain.astype(F32)


def body(
    E, T, CAP,
    tokens, lengths, freqs, g_attn, g_lat, g_mix, g_expert, ids, rw,
    h_qw, h_qr, h_lw, h_kr, h_ab, h_lat, h_rope, h_vw, h_ow, h_gw, h_uw, h_dw,
    out, new_latent, new_rope,
    qw, qr, lw, kr, ab, lat, rope, vw, ow, gw, uw, dw,
    recv1, xs, nin, send2, recv2, qs, send3, recv3, hl, send4, recv4, resid, send5, recv5, xe,
    send6, recv6, ys,
    cos_ref, sin_ref, attn_gain, latent_gain, mix_gain, expert_gain,
    lsem, s1, r1, s2, r2, s3, r3, s4, r4, s5, r5, s6, r6,
):
    ep = lax.axis_index("ep")
    tp = lax.axis_index("tp")
    N = E * T
    me = ep * T + tp
    R, D = tokens.shape
    G = R * T
    Hd, NOPE, LAT = ab.shape
    ROT = kr.shape[0]
    half = ROT // 2
    scale = (NOPE + ROT) ** (-0.5)
    cw = D // T
    slots = E * CAP

    pairs = [
        (h_lw, lw), (h_kr, kr), (h_qw, qw), (h_qr, qr), (h_ab, ab), (h_lat, lat), (h_rope, rope),
        (h_vw, vw), (h_ow, ow), (h_gw, gw), (h_uw, uw), (h_dw, dw),
    ]
    loads = [pltpu.make_async_copy(a, b, lsem.at[i]) for i, (a, b) in enumerate(pairs)]
    c_lw, c_kr, c_qw, c_qr, c_ab, c_lat, c_rope, c_vw, c_ow, c_gw, c_uw, c_dw = loads

    barrier = pltpu.get_barrier_semaphore()

    def greet(d, carry):
        other = lax.rem(me + d, N)
        pl.semaphore_signal(
            barrier, inc=1, device_id=(other // T, lax.rem(other, T)), device_id_type=MESH
        )
        return carry

    lax.fori_loop(1, N, greet, 0)
    for c in loads:
        c.start()
    pl.semaphore_wait(barrier, N - 1)

    def tp_copy(d, src, dst, ss, rs):
        return pltpu.make_async_remote_copy(
            src_ref=src, dst_ref=dst, send_sem=ss, recv_sem=rs,
            device_id=(ep, lax.rem(tp + d, T)), device_id_type=MESH,
        )

    c1 = [tp_copy(d, tokens, recv1.at[tp], s1.at[d], r1.at[d]) for d in range(1, T)]
    for c in c1:
        c.start()
    recv1[tp] = tokens[...]
    for src, dst in (
        (g_attn, attn_gain), (g_lat, latent_gain), (g_mix, mix_gain), (g_expert, expert_gain)
    ):
        rows = src[...].astype(F32)
        for i in range(src.shape[0]):
            wide = src.shape[1]
            dst[:, i * wide:(i + 1) * wide] = rows[i:i + 1]
    row_g = lax.broadcasted_iota(jnp.int32, (G, 1), 0)
    pos = jnp.zeros((G, 1), F32)
    for b in range(G):
        pos = jnp.where(row_g == b, lengths[b].astype(F32), pos)
    angles = pos * freqs[...]
    turns = jnp.floor(angles * (0.5 / np.pi) + 0.5)
    angles = (angles - turns * turn_high) - turns * turn_low
    cos_ref[...] = jnp.cos(angles)
    sin_ref[...] = jnp.sin(angles)
    eye = (
        lax.broadcasted_iota(jnp.int32, (G, G), 1) == lax.broadcasted_iota(jnp.int32, (G, G), 0)
    ).astype(F32)
    topk = ids.shape[0]

    def column(row):
        return jnp.sum(eye * row, axis=1, keepdims=True)

    ide = [column(ids[k:k + 1, :].astype(F32)) for k in range(topk)]
    rwe = [column(rw[k:k + 1, :]) for k in range(topk)]
    lane_e = lax.broadcasted_iota(jnp.int32, (G, E), 1).astype(F32)
    hits = [(ide[k] == lane_e).astype(F32) for k in range(topk)]
    named = sum(hits)
    lower = (
        lax.broadcasted_iota(jnp.int32, (G, G), 1) < lax.broadcasted_iota(jnp.int32, (G, G), 0)
    ).astype(F32)
    before = dot(lower.astype(BF16), named.astype(BF16))
    lane_s = lax.broadcasted_iota(jnp.int32, (G, slots), 1)
    row_s = lax.broadcasted_iota(jnp.int32, (slots, G), 0)
    lane0 = (lax.broadcasted_iota(jnp.int32, (slots, 128), 1) == 0).astype(BF16)
    picks = []
    spread = jnp.zeros((slots, G), F32)
    for k in range(topk):
        rank = jnp.sum(hits[k] * before, axis=1, keepdims=True)
        target = ide[k] * CAP + rank
        picks.append((target.astype(jnp.int32) == lane_s).astype(F32).astype(BF16))
        across = dot_nt(lane0, jnp.broadcast_to(target, (G, 128)).astype(BF16))
        spread = spread + (across.astype(jnp.int32) == row_s).astype(F32)
    spread = spread.astype(BF16)
    send2[...] = jnp.zeros_like(send2)
    for c in c1:
        c.wait()
    for t in range(T):
        xs[t * R:(t + 1) * R, :] = recv1[t].astype(F32)
    nin[...] = norm_rows(xs[...], attn_gain[...]).astype(BF16)

    c_lw.wait()
    c_kr.wait()
    kd = lw.shape[0]
    mine = nin[:, pl.ds(pl.multiple_of(tp * kd, kd), kd)]
    k_lat = dot(mine, lw[...])
    k_rot = dot_nt(mine, kr[...])
    for b in range(G):
        send2[b // R, b % R, Hd:Hd + 1, 0:LAT] = k_lat[b:b + 1]
        send2[b // R, b % R, Hd:Hd + 1, LAT:LAT + ROT] = k_rot[b:b + 1]
    c_qr.wait()
    q_rot = dot(nin[...], qr[...])
    cosv = cos_ref[...]
    sinv = sin_ref[...]
    for h in range(Hd):
        a = q_rot[:, h * ROT:h * ROT + half]
        b2 = q_rot[:, h * ROT + half:(h + 1) * ROT]
        ra = rounded(a * cosv - b2 * sinv)
        rb = rounded(b2 * cosv + a * sinv)
        for b in range(G):
            send2[b // R, b % R, h:h + 1, LAT:LAT + half] = ra[b:b + 1]
            send2[b // R, b % R, h:h + 1, LAT + half:LAT + ROT] = rb[b:b + 1]
    c_qw.wait()
    c_ab.wait()
    for h in range(Hd):
        q = dot(nin[...], qw[:, h * NOPE:(h + 1) * NOPE]).astype(BF16)
        ql = rounded(dot(q, ab[h]))
        for b in range(G):
            send2[b // R, b % R, h:h + 1, 0:LAT] = ql[b:b + 1]
    c2 = [
        tp_copy(d, send2.at[lax.rem(tp + d, T)], recv2.at[tp], s2.at[d], r2.at[d])
        for d in range(1, T)
    ]
    for c in c2:
        c.start()
    recv2[tp] = send2[tp]
    for c in c2:
        c.wait()

    c_lat.wait()
    c_rope.wait()
    for s in range(R):
        raw = sum(recv2[t, s, Hd:Hd + 1, :] for t in range(T))
        nl = norm_rows(raw[:, 0:LAT], latent_gain[...]).astype(BF16)
        cs = cos_ref[pl.ds(tp * R + s, 1), :]
        sn = sin_ref[pl.ds(tp * R + s, 1), :]
        a = raw[:, LAT:LAT + half]
        b2 = raw[:, LAT + half:LAT + ROT]
        nr = jnp.concatenate([a * cs - b2 * sn, b2 * cs + a * sn], axis=1).astype(BF16)
        new_latent[s:s + 1, :] = nl
        new_rope[s:s + 1, :] = nr
        nl = nl.astype(F32)
        nr = nr.astype(F32)
        for t in range(T):
            qs[s, t * Hd:(t + 1) * Hd, :] = recv2[t, s, 0:Hd, :]
        q_l = qs[s, :, 0:LAT]
        q_r = qs[s, :, LAT:LAT + ROT]
        own = (
            jnp.sum(q_l * nl, axis=1, keepdims=True) + jnp.sum(q_r * nr, axis=1, keepdims=True)
        ) * scale
        sc = (dot_nt(q_l.astype(BF16), lat[s]) + dot(q_r.astype(BF16), rope[s])) * scale
        valid = lax.broadcasted_iota(jnp.int32, sc.shape, 1) < lengths[tp * R + s]
        sc = jnp.where(valid, sc, masked_score)
        top = jnp.maximum(jnp.max(sc, axis=1, keepdims=True), own)
        w = jnp.where(valid, jnp.exp(sc - top), 0.0)
        ow_ = jnp.exp(own - top)
        total = jnp.sum(w, axis=1, keepdims=True) + ow_
        o = rounded((dot(w.astype(BF16), lat[s]) + rounded(ow_) * nl) / total)
        for t in range(T):
            for h in range(Hd):
                send3[t, h, s:s + 1, :] = o[t * Hd + h:t * Hd + h + 1]
    c3 = [
        tp_copy(d, send3.at[lax.rem(tp + d, T)], recv3.at[tp], s3.at[d], r3.at[d])
        for d in range(1, T)
    ]
    for c in c3:
        c.start()
    recv3[tp] = send3[tp]
    c_vw.wait()
    c_ow.wait()
    for c in c3:
        c.wait()

    for h in range(Hd):
        for t in range(T):
            hl[h, t * R:(t + 1) * R, :] = recv3[t, h]
    hv = jnp.concatenate(
        [dot(hl[h].astype(BF16), vw[h]).astype(BF16) for h in range(Hd)], axis=1
    )
    c4 = []
    for j in range(T):
        part = dot(hv, ow[:, j * cw:(j + 1) * cw]).astype(BF16)
        send4[j] = part
        recv4[j, tp] = part
        for d in range(1, T):
            c = tp_copy(d, send4.at[j], recv4.at[j, tp], s4.at[j, d], r4.at[j, d])
            c.start()
            c4.append(c)
    for c in c4:
        c.wait()
    for j in range(T):
        total = sum(recv4[j, t].astype(F32) for t in range(T))
        resid[:, j * cw:(j + 1) * cw] = rounded(total)
    res = rounded(xs[...] + norm_rows(resid[...], mix_gain[...]))
    resid[...] = res
    e_in = norm_rows(res, expert_gain[...]).astype(BF16)

    outgoing = dot(spread, e_in)
    for e in range(E):
        send5[e] = outgoing[e * CAP:(e + 1) * CAP].astype(BF16)
    c5 = []
    for d in range(1, E):
        other = lax.rem(ep + d, E)
        c = pltpu.make_async_remote_copy(
            src_ref=send5.at[other], dst_ref=recv5.at[ep], send_sem=s5.at[d], recv_sem=r5.at[d],
            device_id=(other, tp), device_id_type=MESH,
        )
        c.start()
        c5.append(c)
    recv5[ep] = send5[ep]
    c_gw.wait()
    c_uw.wait()
    c_dw.wait()
    for c in c5:
        c.wait()
    for e in range(E):
        xe[e * CAP:(e + 1) * CAP, :] = recv5[e].astype(F32)
    x = xe[...].astype(BF16)
    gate = dot(x, gw[0])
    upward = dot(x, uw[0])
    hidden = (gate / (1.0 + jnp.exp(-gate)) * upward).astype(BF16)
    for j in range(T):
        part = dot(hidden, dw[0, :, j * cw:(j + 1) * cw])
        for e in range(E):
            send6[e * T + j] = part[e * CAP:(e + 1) * CAP].astype(BF16)

    def back(d):
        other = lax.rem(me + d, N)
        return pltpu.make_async_remote_copy(
            src_ref=send6.at[other], dst_ref=recv6.at[me], send_sem=s6.at[d], recv_sem=r6.at[d],
            device_id=(other // T, lax.rem(other, T)), device_id_type=MESH,
        )

    def go(d, carry):
        back(d).start()
        return carry

    def come(d, carry):
        back(d).wait()
        return carry

    lax.fori_loop(1, N, go, 0)
    recv6[me] = send6[me]
    lax.fori_loop(1, N, come, 0)
    for e in range(E):
        ys[e * CAP:(e + 1) * CAP, :] = sum(recv6[e * T + t].astype(F32) for t in range(T))
    y = ys[...].astype(BF16)
    acc = resid[:, pl.ds(pl.multiple_of(tp * cw, cw), cw)]
    add = sum(dot(picks[k], y) * rwe[k] for k in range(topk))
    out[...] = (acc + add).astype(BF16)


def per_device(
    tokens, lengths, latent_cache, rope_cache, attn_gain, query_weight, query_rot_weight,
    latent_weight, key_rot_weight, latent_gain, absorb_weight, value_weight, output_weight,
    mix_gain, expert_gain, gate_weight, up_weight, down_weight, expert_ids, route_weights,
):
    E = lax.axis_size("ep")
    T = lax.axis_size("tp")
    R, D = tokens.shape
    G = R * T
    Hd, NOPE, LAT = absorb_weight.shape
    H = Hd * T
    ROT = key_rot_weight.shape[1]
    CAP = 2 * expert_ids.shape[0] * expert_ids.shape[1] // E
    cw = D // T
    half = ROT // 2
    wq = LAT + -(-ROT // 128) * 128
    freqs = jnp.asarray(rope_base ** (-np.arange(half) / half), F32)[None]
    key_rot_t = key_rot_weight.T
    rope_t = jnp.swapaxes(rope_cache, 1, 2)
    weights = (
        query_weight, query_rot_weight, latent_weight, key_rot_t, absorb_weight,
        latent_cache, rope_t, value_weight, output_weight, gate_weight, up_weight, down_weight,
    )
    vm = pl.BlockSpec(memory_space=pltpu.VMEM)
    sm = pl.BlockSpec(memory_space=pltpu.SMEM)
    anyw = pl.BlockSpec(memory_space=pltpu.HBM)
    dma = pltpu.SemaphoreType.DMA
    N = E * T
    return pl.pallas_call(
        functools.partial(body, E, T, CAP),
        out_shape=(
            jax.ShapeDtypeStruct((G, cw), BF16),
            jax.ShapeDtypeStruct((R, LAT), BF16),
            jax.ShapeDtypeStruct((R, ROT), BF16),
        ),
        in_specs=[vm, sm] + [vm] * 7 + [anyw] * 12,
        out_specs=(vm, vm, vm),
        scratch_shapes=[pltpu.VMEM(w.shape, w.dtype) for w in weights]
        + [
            pltpu.VMEM((T, R, D), BF16),
            pltpu.VMEM((G, D), F32),
            pltpu.VMEM((G, D), BF16),
            pltpu.VMEM((T, R, Hd + 1, wq), F32),
            pltpu.VMEM((T, R, Hd + 1, wq), F32),
            pltpu.VMEM((R, H, wq), F32),
            pltpu.VMEM((T, Hd, R, LAT), F32),
            pltpu.VMEM((T, Hd, R, LAT), F32),
            pltpu.VMEM((Hd, G, LAT), F32),
            pltpu.VMEM((T, G, cw), BF16),
            pltpu.VMEM((T, T, G, cw), BF16),
            pltpu.VMEM((G, D), F32),
            pltpu.VMEM((E, CAP, D), BF16),
            pltpu.VMEM((E, CAP, D), BF16),
            pltpu.VMEM((E * CAP, D), F32),
            pltpu.VMEM((N, CAP, cw), BF16),
            pltpu.VMEM((N, CAP, cw), BF16),
            pltpu.VMEM((E * CAP, cw), F32),
            pltpu.VMEM((G, half), F32),
            pltpu.VMEM((G, half), F32),
            pltpu.VMEM((1, D), F32),
            pltpu.VMEM((1, LAT), F32),
            pltpu.VMEM((1, D), F32),
            pltpu.VMEM((1, D), F32),
            dma((12,)),
            dma((T,)), dma((T,)), dma((T,)), dma((T,)), dma((T,)), dma((T,)),
            dma((T, T)), dma((T, T)), dma((E,)), dma((E,)), dma((N,)), dma((N,)),
        ],
        compiler_params=pltpu.CompilerParams(
            collective_id=0, has_side_effects=True, vmem_limit_bytes=63 * 1024 * 1024
        ),
    )(
        tokens, lengths, freqs, fold(attn_gain), fold(latent_gain), fold(mix_gain),
        fold(expert_gain), expert_ids.T, route_weights.T, *weights,
    )


def solution(mesh):
    placed = (
        P(("ep", "tp"), None), P("ep"), P(("ep", "tp"), None, None), P(("ep", "tp"), None, None),
        P(), P(None, "tp"), P(None, "tp"), P("tp", None), P("tp", None), P(),
        P("tp", None, None), P("tp", None, None), P("tp", None), P(), P(),
        P("ep", None, "tp"), P("ep", None, "tp"), P("ep", "tp", None), P("ep", None), P("ep", None),
    )
    return jax.shard_map(
        per_device,
        mesh=mesh,
        in_specs=placed,
        out_specs=(P("ep", "tp"), P(("ep", "tp"), None), P(("ep", "tp"), None)),
        check_vma=False,
    )
```
